32 devices in a mesh: sp: 8 (over z, x), tp: 4 (over y, core).
Axes of the slice: x: 2, y: 2, z: 4, core: 2. Of those that a mesh axis runs over, the one named last changes fastest.
Arguments:
- residual_in: bfloat16 [8192, 2048], P(('sp', 'tp')), may hold values from -6 to 6
- gate_outer: bfloat16 [8192, 1024], P('sp', 'tp'), may hold values from -6 to 6
- gate_inner: bfloat16 [8192, 1024], P('sp', 'tp'), may hold values from -6 to 6
- conv_input: bfloat16 [8192, 1024], P('sp', 'tp'), may hold values from -6 to 6
- conv_taps: bfloat16 [3, 1024], P(None, 'tp'), may hold values from -5 to 5
- norm_gain: bfloat16 [1024], P('tp'), may hold values from 0.099609375 to 1.8984375
- out_weight: bfloat16 [1024, 2048], P('tp'), may hold values from -0.1875 to 0.1875
- moe_gain: bfloat16 [2048], replicated, may hold values from 0.099609375 to 1.8984375
- expert_ids: int32 [8192, 2], P(('sp', 'tp')), may hold values from 0 to 7, all different within a row; in each aligned block of 256 rows (0 to 255, 256 to 511, ...) at most 128 rows name the same one
- group_prob: float32 [8192], P(('sp', 'tp')), may hold values from 0.3 to 1
- route_prob: float32 [8192, 2], P(('sp', 'tp')), may hold values from 0.1 to 1
- expert_gate: bfloat16 [8, 2048, 512], P('sp'), may hold values from -0.125 to 0.125
- expert_up: bfloat16 [8, 2048, 512], P('sp'), may hold values from -0.125 to 0.125
- expert_down: bfloat16 [8, 512, 2048], P('sp'), may hold values from -0.25 to 0.25
Outputs:
- layer_out: bfloat16 [8192, 2048], P(('sp', 'tp'))
The draws below stay inside these ranges and needn't reach their ends.
Inputs may be any that keep to these rules, and one draw needn't show every extreme that they name: `expert_ids`: each row names 2 different experts. Within the rows of one device (aligned blocks of 256 rows) no expert is named more than 128 times.
All inputs are finite; a program needn't handle non-finite values.
Results may differ from the reference program's by a relative error of at most 0.0075.
Values may be sent and summed in bfloat16 or wider, within the bound.
No kernel may reach another device: no remote copies, remote signals or barrier semaphores. Data moves between devices by JAX's collectives and lax.ppermute only.
A program may use at most 64 MiB of HBM per device.

```python
import math
import jax
import jax.numpy as jnp
import numpy as np
from jax import lax

D = 2048
CONV = 1024
FE = 512
KW = 3
TOPK = 2
ROWS_DEV = 256
TOKENS = 8192
EXPERTS = 8
CAPACITY = 128


def draw_conv_taps(key, part):
    first, second = jax.random.split(key)
    base = jnp.clip(jax.random.normal(first, (KW, CONV), jnp.float32), -3.0, 3.0) / jnp.sqrt(jnp.float32(KW))
    levels = jnp.array([0.35, 0.7, 1.4, 2.8], jnp.float32)
    shuffled = levels[jax.random.permutation(second, 4)]
    quarter = jnp.arange(CONV, dtype=jnp.int32) * 4 // CONV
    return (base * shuffled[quarter][None, :]).astype(jnp.bfloat16)


def shard_levels(stream_key, extent, pieces, low, high):
    factor_of, own = 1.0, jax.random.fold_in(stream_key, 6)
    for position, blocks in pieces:
        steps = jnp.exp(jax.random.uniform(jax.random.fold_in(own, position), (blocks,), jnp.float32, low / len(pieces), high / len(pieces)))
        factor_of = factor_of * jnp.repeat(steps, extent[position] // blocks).reshape([-1 if axis == position else 1 for axis in range(len(extent))])
    return factor_of


def assign_block(key, own, number, rows, number_of, top, reach, slope):
    ranking = jax.random.permutation(key, number_of)
    heavy_load, common = shares(number_of, rows * top, reach, slope, True), shares(number_of, rows * top, reach, slope, False)
    places = jnp.arange(number_of)

    def named(sizes, turn):
        used = int((sizes > 0).sum())
        fixed = max(1, used // 4)
        moved = fixed + (places - fixed + turn * (used - fixed)) % max(1, number_of - fixed)
        return jnp.zeros((number_of,), jnp.int32).at[ranking[jnp.where(places < fixed, places, moved)]].set(jnp.asarray(sizes, jnp.int32))

    sizes = jnp.where(number % 4 == 0, named(heavy_load, number // 4), named(common, number - number // 4 - 1))
    mixed = jax.random.permutation(jax.random.fold_in(own, 3), number_of)
    donor, receiver = mixed[0:number_of // 2 * 2:2], mixed[1:number_of // 2 * 2:2]
    margin = jnp.minimum(sizes[donor] - 1, reach - sizes[receiver]) // 2
    margin = jnp.where((donor == ranking[0]) | (receiver == ranking[0]) | (sizes[receiver] == 0), 0, jnp.maximum(margin, 0))
    moved = jax.random.randint(jax.random.fold_in(own, 4), (number_of // 2,), 0, 1 << 20) % (margin + 1)
    sizes = sizes.at[donor].add(-moved).at[receiver].add(moved)
    items = jnp.searchsorted(jnp.cumsum(sizes), jnp.arange(rows * top), side="right").astype(jnp.int32)
    listing = items.reshape(top, rows).T
    listing = listing[jax.random.permutation(jax.random.fold_in(own, 1), rows)]
    turn = jax.random.randint(jax.random.fold_in(own, 2), (rows, 1), 0, top)
    return jnp.take_along_axis(listing, (jnp.arange(top)[None, :] + turn) % top, axis=1)


def shares(count, total, reach, slope, full):
    loads = [(1 << 20) // math.isqrt(rank ** slope) + 1 for rank in range(1, count + 1)]
    largest = reach if full else min(reach, max(-(-total // count), total * loads[0] // sum(loads)))
    least = 1 if total - largest >= count - 1 else 0
    holding, rest = [largest] + [least] * (count - 1), total - largest - least * (count - 1)
    while rest > 0:
        candidates = [i for i in range(1, count) if holding[i] < largest] or [i for i in range(1, count) if holding[i] < reach]
        pool, left = sum([loads[i] for i in candidates]), rest
        for i in candidates:
            more = min(reach - holding[i], max(1, left * loads[i] // pool), rest)
            holding[i] = holding[i] + more
            rest = rest - more
    return np.array(holding)


def normal_values(stream_key, dims, deviation, most, cuts=(), kind=jnp.bfloat16):
    values = jax.random.normal(stream_key, dims, jnp.float32) * deviation
    if len(cuts) > 0:
        values = shard_levels(stream_key, dims, cuts, -0.22, 0.18) * values
    return jnp.clip(values, min=-most, max=most).astype(kind)


def setup_inputs(seed: int = 0) -> dict:
    key_list = jax.random.split(jax.random.key(seed), 15)
    residual_in = normal_values(key_list[0], (TOKENS, D), 1.0, 6.0, ((0, 32),))
    gate_outer = normal_values(key_list[1], (TOKENS, CONV), 1.0, 6.0, ((0, 8), (1, 4)))
    gate_inner = normal_values(key_list[2], (TOKENS, CONV), 1.0, 6.0, ((0, 8), (1, 4)))
    conv_input = normal_values(key_list[3], (TOKENS, CONV), 1.0, 6.0, ((0, 8), (1, 4)))
    conv_taps = draw_conv_taps(jax.random.fold_in(key_list[14], 71), 0)
    norm_gain = jnp.clip(1.0 + 0.18 * jax.random.normal(key_list[5], (CONV,), jnp.float32), 0.099609375, 1.8984375).astype(jnp.bfloat16)
    out_weight = normal_values(key_list[6], (CONV, D), CONV ** -0.5, 0.1875, ((0, 4),))
    moe_gain = jnp.clip(1.0 + 0.18 * jax.random.normal(key_list[7], (D,), jnp.float32), 0.099609375, 1.8984375).astype(jnp.bfloat16)
    expert_ids_keys = jax.random.split(jax.random.fold_in(key_list[8], 1), TOKENS // ROWS_DEV)
    expert_ids_turns = jax.random.permutation(jax.random.fold_in(key_list[8], 3), TOKENS // ROWS_DEV)
    expert_ids = jax.vmap(lambda own, number: assign_block(jax.random.fold_in(key_list[8], 2), own, number, ROWS_DEV, EXPERTS, TOPK, CAPACITY, 2))(expert_ids_keys, expert_ids_turns).reshape((TOKENS, TOPK))
    group_prob = jnp.clip(0.3 + 0.7 * jax.random.uniform(key_list[9], (TOKENS,), jnp.float32) ** shard_levels(key_list[9], (TOKENS,), ((0, 32),), -0.2, 0.2), 0.3, 1.0)
    route_prob = jnp.clip(0.1 + 0.9 * jax.random.uniform(key_list[10], (TOKENS, TOPK), jnp.float32) ** shard_levels(key_list[10], (TOKENS, TOPK), ((0, 32),), -0.2, 0.2), 0.1, 1.0)
    expert_gate = normal_values(key_list[11], (EXPERTS, D, FE), D ** -0.5, 0.125, ((0, 8),))
    expert_up = normal_values(key_list[12], (EXPERTS, D, FE), D ** -0.5, 0.125, ((0, 8),))
    expert_down = normal_values(key_list[13], (EXPERTS, FE, D), FE ** -0.5, 0.25, ((0, 8),))
    return dict(residual_in=residual_in, gate_outer=gate_outer, gate_inner=gate_inner, conv_input=conv_input, conv_taps=conv_taps, norm_gain=norm_gain, out_weight=out_weight, moe_gain=moe_gain, expert_ids=expert_ids, group_prob=group_prob, route_prob=route_prob, expert_gate=expert_gate, expert_up=expert_up, expert_down=expert_down)


EPSILON = 1e-06

def rms_norm(values, gain):
    floats = values.astype(jnp.float32)
    factor = lax.rsqrt(lax.optimization_barrier(jnp.mean(floats * floats, axis=-1, keepdims=True)) + EPSILON)
    return floats * factor * gain.astype(jnp.float32)

def reference(residual_in, gate_outer, gate_inner, conv_input, conv_taps, norm_gain, out_weight, moe_gain, expert_ids, group_prob, route_prob, expert_gate, expert_up, expert_down):
    inner = gate_inner.astype(jnp.float32) * conv_input.astype(jnp.float32)
    padded = jnp.concatenate([jnp.zeros((KW - 1, CONV), jnp.float32), inner], axis=0)
    tap_f = conv_taps.astype(jnp.float32)
    filtered = jnp.zeros((TOKENS, CONV), jnp.float32)
    for offset in range(KW):
        filtered = filtered + tap_f[offset][None, :] * padded[offset:offset + TOKENS]
    mixed = (gate_outer.astype(jnp.float32) * filtered).astype(jnp.bfloat16)
    normed = rms_norm(mixed, norm_gain).astype(jnp.bfloat16)
    residual = (residual_in.astype(jnp.float32) + jnp.dot(normed, out_weight, preferred_element_type=jnp.float32)).astype(jnp.bfloat16)
    routed_in = rms_norm(residual, moe_gain).astype(jnp.bfloat16)
    slots = TOKENS * TOPK
    block_rows = 256
    flat_e = expert_ids.reshape(-1).astype(jnp.int32)
    order = jnp.argsort(flat_e, stable=True).astype(jnp.int32)
    sorted_e = flat_e[order]
    counts = jnp.bincount(flat_e, length=EXPERTS).astype(jnp.int32)
    padded_counts = (counts + block_rows - 1) // block_rows * block_rows
    pad_end = jnp.cumsum(padded_counts).astype(jnp.int32)
    pad_start = pad_end - padded_counts
    seg_start = (jnp.cumsum(counts) - counts).astype(jnp.int32)
    dest = pad_start[sorted_e] + jnp.arange(slots, dtype=jnp.int32) - seg_start[sorted_e]
    block_count = (slots + block_rows - 1) // block_rows + EXPERTS
    total_rows = block_count * block_rows
    buffer_slot = jnp.full((total_rows,), slots, jnp.int32).at[dest].set(order)
    block_expert = jnp.minimum(jnp.searchsorted(pad_end, jnp.arange(block_count, dtype=jnp.int32) * block_rows, side='right'), EXPERTS - 1).astype(jnp.int32)
    rows_pad = jnp.concatenate([routed_in, jnp.zeros((1, D), jnp.bfloat16)], axis=0)

    def one_block(items):
        slot_ids, expert = items
        token_row = jnp.where(slot_ids < slots, slot_ids // TOPK, TOKENS)
        block_in = rows_pad[token_row]
        gate_act = jnp.dot(block_in, expert_gate[expert], preferred_element_type=jnp.float32)
        up_act = jnp.dot(block_in, expert_up[expert], preferred_element_type=jnp.float32)
        hidden = (jax.nn.silu(gate_act) * up_act).astype(jnp.bfloat16)
        return jnp.dot(hidden, expert_down[expert], preferred_element_type=jnp.float32).astype(jnp.bfloat16)
    results = lax.map(one_block, (buffer_slot.reshape(block_count, block_rows), block_expert)).reshape(total_rows, D)
    slot_out = jnp.zeros((slots + 1, D), jnp.bfloat16).at[buffer_slot].set(results)[:slots]
    weights = group_prob[:, None] * route_prob / lax.optimization_barrier(jnp.sum(route_prob, axis=1, keepdims=True))
    expert_sum = lax.optimization_barrier(jnp.sum(slot_out.reshape(TOKENS, TOPK, D).astype(jnp.float32) * weights[:, :, None], axis=1))
    return (residual.astype(jnp.float32) + expert_sum).astype(jnp.bfloat16)
```

```python
import jax
import jax.numpy as jnp
from jax import lax
from jax.sharding import PartitionSpec as P

EPSILON = 1e-06


def from_behind(shard, axis, by):
    devices = lax.axis_size(axis)
    pairs = [(i, i + by) for i in range(devices) if 0 <= i + by < devices]
    return lax.ppermute(shard, axis, pairs)


def swap(shard, axis, bit):
    devices = lax.axis_size(axis)
    return lax.ppermute(shard, axis, [(i, i ^ bit) for i in range(devices)])


def rms_norm(values, gain):
    floats = values.astype(jnp.float32)
    factor = lax.rsqrt(jnp.mean(floats * floats, axis=-1, keepdims=True) + EPSILON)
    return floats * factor * gain.astype(jnp.float32)


def mixer(gate_outer, gate_inner, conv_input, conv_taps):
    seq_rows, channels = conv_input.shape
    taps_count = conv_taps.shape[0]
    halo = taps_count - 1
    tail = slice(seq_rows - halo, seq_rows)
    earlier = from_behind(
        gate_inner[tail].astype(jnp.float32) * conv_input[tail].astype(jnp.float32), "sp", 1
    )
    inner = gate_inner.astype(jnp.float32) * conv_input.astype(jnp.float32)
    padded = jnp.concatenate([earlier, inner], axis=0)
    tap_f = conv_taps.astype(jnp.float32)
    filtered = jnp.zeros((seq_rows, channels), jnp.float32)
    for offset in range(taps_count):
        filtered = filtered + tap_f[offset][None, :] * padded[offset : offset + seq_rows]
    return (gate_outer.astype(jnp.float32) * filtered).astype(jnp.bfloat16)


def gather_tp(piece):
    index = lax.axis_index("tp")
    count = lax.axis_size("tp")
    held = [(0, piece)]
    bit = count // 2
    while bit:
        held = held + [(other ^ bit, swap(block, "tp", bit)) for other, block in held]
        bit //= 2
    whole = jnp.zeros((count,) + piece.shape, piece.dtype)
    for other, block in held:
        whole = lax.dynamic_update_slice_in_dim(whole, block[None], index ^ other, 0)
    return whole


def route_slots(routed_in, residual, expert_ids, weights, expert_gate, expert_up, expert_down):
    tok_rows, width = routed_in.shape
    top_count = expert_ids.shape[1]
    local_count = expert_gate.shape[0]
    group_count = lax.axis_size("sp")
    experts_all = local_count * group_count
    capacity = 2 * tok_rows * top_count // experts_all
    slots = tok_rows * top_count
    flat_e = expert_ids.reshape(-1)
    one_hot = (flat_e[:, None] == jnp.arange(experts_all, dtype=jnp.int32)[None, :]).astype(
        jnp.int32
    )
    slot_rank = jnp.sum((jnp.cumsum(one_hot, axis=0) - 1) * one_hot, axis=1)
    owner_dev = flat_e // local_count
    local_slot = flat_e % local_count
    position = (local_slot * group_count + owner_dev) * capacity + slot_rank
    source_slot = (
        jnp.full((experts_all * capacity,), slots, jnp.int32)
        .at[position]
        .set(jnp.arange(slots, dtype=jnp.int32))
    )
    rows_pad = jnp.concatenate([routed_in, jnp.zeros((1, width), jnp.bfloat16)], axis=0)
    outgoing = rows_pad[source_slot // top_count].reshape(local_count, group_count, capacity, width)
    arrived = lax.all_to_all(outgoing, "sp", split_axis=1, concat_axis=1, tiled=True)
    gate_act = jnp.einsum(
        "esrd,edf->esrf", arrived, expert_gate, preferred_element_type=jnp.float32
    )
    up_act = jnp.einsum("esrd,edf->esrf", arrived, expert_up, preferred_element_type=jnp.float32)
    hidden = (jax.nn.silu(gate_act) * up_act).astype(jnp.bfloat16)
    result = jnp.einsum(
        "esrf,efd->esrd", hidden, expert_down, preferred_element_type=jnp.float32
    ).astype(jnp.bfloat16)
    returned = lax.all_to_all(result, "sp", split_axis=1, concat_axis=1, tiled=True)
    slot_out = returned.reshape(-1, width)[position].reshape(tok_rows, top_count, width)
    expert_sum = jnp.sum(slot_out.astype(jnp.float32) * weights[:, :, None], axis=1)
    return (residual.astype(jnp.float32) + expert_sum).astype(jnp.bfloat16)


def expert_rows(rows, row_weight, gate, up, down):
    gate_act = jnp.dot(rows, gate, preferred_element_type=jnp.float32)
    up_act = jnp.dot(rows, up, preferred_element_type=jnp.float32)
    hidden = (jax.nn.silu(gate_act) * up_act).astype(jnp.bfloat16)
    result = jnp.dot(hidden, down, preferred_element_type=jnp.float32).astype(jnp.bfloat16)
    return result.astype(jnp.float32) * row_weight[:, None]


def fetch_expert(expert_gate, expert_up, expert_down):
    parts = lax.axis_size("tp")
    index = lax.axis_index("tp")
    far = lax.axis_size("sp") // 2
    depth, hidden = expert_gate.shape[1:]
    width = expert_down.shape[2]
    deep, wide = depth // parts, width // parts
    first = jnp.stack(
        [
            lax.dynamic_slice_in_dim(expert_gate[0], index * deep, deep, 0),
            lax.dynamic_slice_in_dim(expert_up[0], index * deep, deep, 0),
        ]
    )
    second = lax.dynamic_slice_in_dim(expert_down[0], index * (hidden // parts), hidden // parts, 0)
    first = gather_tp(swap(first, "sp", far))
    second = gather_tp(swap(second, "sp", far))
    return (
        first[:, 0].reshape(depth, hidden),
        first[:, 1].reshape(depth, hidden),
        second.reshape(hidden, width),
    )


def share_square(routed_in, residual, expert_ids, weights, expert_gate, expert_up, expert_down):
    rows = routed_in.shape[0]
    half = rows // 2
    index = lax.axis_index("sp")
    count = lax.axis_size("sp")
    across, along = 1, 2
    far_gate, far_up, far_down = fetch_expert(expert_gate, expert_up, expert_down)

    names = jnp.arange(count, dtype=jnp.int32)
    dense = jnp.sum(
        jnp.where(expert_ids[None] == names[:, None, None], weights[None], 0.0), axis=2
    )
    dense_of = {0: dense}
    dense_of[across] = swap(dense, "sp", across)
    dense_of[along] = swap(dense, "sp", along)
    dense_of[across | along] = swap(dense, "sp", across | along)

    low, high = routed_in[:half], routed_in[half:]
    x_high = swap(high, "sp", across)
    z_low = swap(low, "sp", along)
    x_low = swap(low, "sp", across)
    z_high = swap(high, "sp", along)
    d_low = swap(z_low, "sp", across)
    d_high = swap(x_high, "sp", along)

    near = (expert_gate[0], expert_up[0], expert_down[0])
    far = (far_gate, far_up, far_down)

    def partial(block, member):
        near_w = lax.dynamic_index_in_dim(dense_of[member], index, 0, keepdims=False)
        far_w = lax.dynamic_index_in_dim(dense_of[member], index ^ (count // 2), 0, keepdims=False)
        return expert_rows(block, near_w, *near) + expert_rows(block, far_w, *far)

    mine = partial(routed_in, 0)
    for_x = partial(jnp.concatenate([x_low, x_high]), across)
    for_z = partial(jnp.concatenate([z_low, z_high]), along)
    for_d = partial(jnp.concatenate([d_low, d_high]), across | along).astype(jnp.bfloat16)
    from_x_low = swap(for_x[:half].astype(jnp.bfloat16), "sp", across)
    from_z_high = swap(for_z[half:].astype(jnp.bfloat16), "sp", along)
    via_x = swap(for_d[:half], "sp", across)
    via_z = swap(for_d[half:], "sp", along)
    from_z_low = swap((for_z[:half] + via_x.astype(jnp.float32)).astype(jnp.bfloat16), "sp", along)
    from_x_high = swap((for_x[half:] + via_z.astype(jnp.float32)).astype(jnp.bfloat16), "sp", across)
    others = jnp.concatenate([from_x_low, from_x_high]).astype(jnp.float32) + jnp.concatenate(
        [from_z_low, from_z_high]
    ).astype(jnp.float32)
    return (residual.astype(jnp.float32) + (mine + others)).astype(jnp.bfloat16)


def body(
    residual_in,
    gate_outer,
    gate_inner,
    conv_input,
    conv_taps,
    norm_gain,
    out_weight,
    moe_gain,
    expert_ids,
    group_prob,
    route_prob,
    expert_gate,
    expert_up,
    expert_down,
):
    mixed_out = mixer(gate_outer, gate_inner, conv_input, conv_taps)
    gathered = lax.all_to_all(mixed_out, "tp", split_axis=0, concat_axis=1, tiled=True)
    full_weight = gather_tp(out_weight).reshape(-1, out_weight.shape[1])
    full_gain = lax.all_gather(norm_gain, "tp", axis=0, tiled=True)
    normed = rms_norm(gathered, full_gain).astype(jnp.bfloat16)
    projected = jnp.dot(normed, full_weight, preferred_element_type=jnp.float32)
    residual = (residual_in.astype(jnp.float32) + projected).astype(jnp.bfloat16)
    routed_in = rms_norm(residual, moe_gain).astype(jnp.bfloat16)
    weights = group_prob[:, None] * route_prob / jnp.sum(route_prob, axis=1, keepdims=True)
    local_count, group_count = expert_gate.shape[0], lax.axis_size("sp")
    few = local_count * group_count <= 4 * expert_ids.shape[1]
    square = local_count == 1 and group_count % 8 == 0
    path = share_square if few and square else route_slots
    return path(routed_in, residual, expert_ids, weights, expert_gate, expert_up, expert_down)


def solution(mesh):
    in_specs = (
        P(("sp", "tp"), None),
        P("sp", "tp"),
        P("sp", "tp"),
        P("sp", "tp"),
        P(None, "tp"),
        P("tp"),
        P("tp", None),
        P(),
        P(("sp", "tp"), None),
        P(("sp", "tp")),
        P(("sp", "tp"), None),
        P("sp", None, None),
        P("sp", None, None),
        P("sp", None, None),
    )
    out_specs = P(("sp", "tp"), None)
    return jax.shard_map(body, mesh=mesh, in_specs=in_specs, out_specs=out_specs, check_vma=False)
```

```python
import functools

import jax
import jax.numpy as jnp
from jax import lax
from jax.experimental import pallas as pl
from jax.experimental.pallas import tpu as pltpu
from jax.sharding import PartitionSpec as P


EPSILON = 1e-06


def from_behind(shard, axis, by):
    devices = lax.axis_size(axis)
    pairs = [(i, i + by) for i in range(devices) if 0 <= i + by < devices]
    return lax.ppermute(shard, axis, pairs)


def swap(shard, axis, bit):
    devices = lax.axis_size(axis)
    return lax.ppermute(shard, axis, [(i, i ^ bit) for i in range(devices)])


def rms_norm(values, gain):
    floats = values.astype(jnp.float32)
    factor = lax.rsqrt(jnp.mean(floats * floats, axis=-1, keepdims=True) + EPSILON)
    return floats * factor * gain.astype(jnp.float32)


def mixer(gate_outer, gate_inner, conv_input, conv_taps):
    seq_rows, channels = conv_input.shape
    taps_count = conv_taps.shape[0]
    halo = taps_count - 1
    tail = slice(seq_rows - halo, seq_rows)
    earlier = from_behind(
        gate_inner[tail].astype(jnp.float32) * conv_input[tail].astype(jnp.float32), "sp", 1
    )
    inner = gate_inner.astype(jnp.float32) * conv_input.astype(jnp.float32)
    padded = jnp.concatenate([earlier, inner], axis=0)
    tap_f = conv_taps.astype(jnp.float32)
    filtered = jnp.zeros((seq_rows, channels), jnp.float32)
    for offset in range(taps_count):
        filtered = filtered + tap_f[offset][None, :] * padded[offset : offset + seq_rows]
    return (gate_outer.astype(jnp.float32) * filtered).astype(jnp.bfloat16)


def spread_tp(piece, hold=None):
    other = swap(piece, "tp", 2)
    near = swap(piece, "tp", 1)
    held = other if hold is None else after(other, hold)
    return [piece, near, held, swap(held, "tp", 1)]


def after(values, first):
    return lax.optimization_barrier((values, first))[0]


def call(kernel, outs, scratch, copies, flops, *operands, limit=40):
    at = jnp.stack([lax.axis_index("tp"), lax.axis_index("sp")]).astype(jnp.int32)
    in_vmem = pl.BlockSpec(memory_space=pltpu.VMEM)
    anywhere = pl.BlockSpec(memory_space=pltpu.HBM)
    moved = sum(a.size * a.dtype.itemsize for a in operands)
    return pl.pallas_call(
        kernel,
        out_shape=outs,
        in_specs=[pl.BlockSpec(memory_space=pltpu.SMEM)]
        + [anywhere] * copies
        + [in_vmem] * (len(operands) - copies),
        out_specs=[in_vmem] * len(outs),
        scratch_shapes=scratch + [pltpu.SemaphoreType.DMA((copies,))],
        compiler_params=pltpu.CompilerParams(vmem_limit_bytes=limit * 2**20),
        cost_estimate=pl.CostEstimate(flops=flops, bytes_accessed=moved, transcendentals=0),
    )(at, *operands)


def row_part(ref, index, count):
    return ref.at[pl.ds(pl.multiple_of(index * count, count), count)]


def project_kernel(at, w0, w1, w2, w3, res_in, mixed, moe_gain, residual, low, high, weight, held, sems):
    pieces = (w0, w1, w2, w3)
    deep, rows = w0.shape[0], res_in.shape[0]
    copies = [
        pltpu.make_async_copy(w, row_part(weight, at[0] ^ j, deep), sems.at[j])
        for j, w in enumerate(pieces)
    ]
    copies.append(pltpu.make_async_copy(res_in, held, sems.at[len(pieces)]))
    for copy in copies:
        copy.start()
    count, width = mixed.shape[0], mixed.shape[2]
    floats = [mixed[j, 0:rows].astype(jnp.float32) for j in range(count)]
    total = sum(jnp.sum(f * f, axis=-1, keepdims=True) for f in floats)
    factor = lax.rsqrt(total / (count * width) + EPSILON)
    normed = [
        (floats[j] * factor * mixed[j, rows : rows + 1].astype(jnp.float32)).astype(jnp.bfloat16)
        for j in range(count)
    ]
    for copy in copies:
        copy.wait()
    summed = jnp.dot(
        jnp.concatenate(normed, axis=1), weight[...], preferred_element_type=jnp.float32
    )
    new = (held[...].astype(jnp.float32) + summed).astype(jnp.bfloat16)
    residual[...] = new
    floats = new.astype(jnp.float32)
    scale = lax.rsqrt(jnp.mean(floats * floats, axis=-1, keepdims=True) + EPSILON)
    routed = (floats * scale * moe_gain[...].astype(jnp.float32)).astype(jnp.bfloat16)
    half = rows // 2
    low[...] = routed[:half]
    high[...] = routed[half:]


def project(mixed, pieces, res_in, moe_gain):
    rows, width = res_in.shape
    outs = [
        jax.ShapeDtypeStruct((rows, width), jnp.bfloat16),
        jax.ShapeDtypeStruct((rows // 2, width), jnp.bfloat16),
        jax.ShapeDtypeStruct((rows // 2, width), jnp.bfloat16),
    ]
    depth = mixed.shape[0] * mixed.shape[2]
    scratch = [pltpu.VMEM((depth, width), jnp.bfloat16), pltpu.VMEM((rows, width), jnp.bfloat16)]
    return call(
        project_kernel, outs, scratch, 5, 2 * rows * width * depth,
        *pieces, res_in, mixed, moe_gain[None],
    )


def hidden_kernel(gates, blocks, step, at, *refs):
    weights, rows = refs[: 2 * gates], refs[2 * gates : 2 * gates + blocks]
    out, gate, up, held, sems = refs[2 * gates + blocks :]
    deep = weights[0].shape[0]

    def fetch(n):
        if gates == 1:
            place = (gate, up)[n]
        else:
            place = row_part((gate, up)[n // gates], at[0] ^ (n % gates), deep)
        return pltpu.make_async_copy(weights[n], place, sems.at[n])

    loads, position = [], 0
    for n, x in enumerate(rows):
        place = held.at[position : position + x.shape[0]]
        loads.append((position, pltpu.make_async_copy(x, place, sems.at[2 * gates + n])))
        position += x.shape[0]
    fetches = [fetch(n) for n in range(2 * gates)]
    for copy in fetches[:gates]:
        copy.start()
    for begin, copy in loads:
        copy.start()
        if begin == 0:
            for other in fetches[gates:]:
                other.start()
    for begin in range(0, position, step):
        for first, copy in loads:
            if begin <= first < begin + step:
                copy.wait()
        if begin == 0:
            for copy in fetches[:gates]:
                copy.wait()
        span = slice(begin, begin + step)
        g = jnp.dot(held[span], gate[...], preferred_element_type=jnp.float32)
        if begin == 0:
            for copy in fetches[gates:]:
                copy.wait()
        u = jnp.dot(held[span], up[...], preferred_element_type=jnp.float32)
        out[span] = (g * jax.nn.sigmoid(g) * u).astype(jnp.bfloat16)


def hidden_of(blocks, gate, up):
    rows, depth = sum(b.shape[0] for b in blocks), blocks[0].shape[1]
    wide = gate[0].shape[1]
    kernel = functools.partial(hidden_kernel, len(gate), len(blocks), 2 * blocks[0].shape[0])
    scratch = [pltpu.VMEM((depth, wide), jnp.bfloat16)] * 2 + [pltpu.VMEM((rows, depth), jnp.bfloat16)]
    (out,) = call(
        kernel, [jax.ShapeDtypeStruct((rows, wide), jnp.bfloat16)], scratch,
        2 * len(gate) + len(blocks), 4 * rows * depth * wide, *gate, *up, *blocks,
    )
    return out


def route_slots(routed_in, residual, expert_ids, weights, expert_gate, expert_up, expert_down):
    tok_rows, width = routed_in.shape
    top_count = expert_ids.shape[1]
    local_count = expert_gate.shape[0]
    group_count = lax.axis_size("sp")
    experts_all = local_count * group_count
    capacity = 2 * tok_rows * top_count // experts_all
    slots = tok_rows * top_count
    flat_e = expert_ids.reshape(-1)
    one_hot = (flat_e[:, None] == jnp.arange(experts_all, dtype=jnp.int32)[None, :]).astype(
        jnp.int32
    )
    slot_rank = jnp.sum((jnp.cumsum(one_hot, axis=0) - 1) * one_hot, axis=1)
    owner_dev = flat_e // local_count
    local_slot = flat_e % local_count
    position = (local_slot * group_count + owner_dev) * capacity + slot_rank
    source_slot = (
        jnp.full((experts_all * capacity,), slots, jnp.int32)
        .at[position]
        .set(jnp.arange(slots, dtype=jnp.int32))
    )
    rows_pad = jnp.concatenate([routed_in, jnp.zeros((1, width), jnp.bfloat16)], axis=0)
    outgoing = rows_pad[source_slot // top_count].reshape(local_count, group_count, capacity, width)
    arrived = lax.all_to_all(outgoing, "sp", split_axis=1, concat_axis=1, tiled=True)
    gate_act = jnp.einsum(
        "esrd,edf->esrf", arrived, expert_gate, preferred_element_type=jnp.float32
    )
    up_act = jnp.einsum("esrd,edf->esrf", arrived, expert_up, preferred_element_type=jnp.float32)
    hidden = (jax.nn.silu(gate_act) * up_act).astype(jnp.bfloat16)
    result = jnp.einsum(
        "esrf,efd->esrd", hidden, expert_down, preferred_element_type=jnp.float32
    ).astype(jnp.bfloat16)
    returned = lax.all_to_all(result, "sp", split_axis=1, concat_axis=1, tiled=True)
    slot_out = returned.reshape(-1, width)[position].reshape(tok_rows, top_count, width)
    expert_sum = jnp.sum(slot_out.astype(jnp.float32) * weights[:, :, None], axis=1)
    return (residual.astype(jnp.float32) + expert_sum).astype(jnp.bfloat16)


def column_of(weights, index):
    lanes = lax.broadcasted_iota(jnp.int32, weights.shape, 1)
    return jnp.sum(jnp.where(lanes == index, weights[...], 0.0), axis=-1, keepdims=True)


def down_kernel(groups, column, at, near, *refs):
    pieces, refs = refs[:4], refs[4:]
    near_w, far_w, sems = refs[-3:]
    members, outs = len(groups), refs[-3 - len(groups) : -3]
    wide, extent = pieces[0].shape[1], near_w.shape[1]
    copies = [pltpu.make_async_copy(near.at[:, column : column + extent], near_w, sems.at[0])]
    for j, piece in enumerate(pieces):
        place = pl.ds(pl.multiple_of((at[0] ^ j) * wide, wide), wide)
        copies.append(pltpu.make_async_copy(piece, far_w.at[:, place], sems.at[1 + j]))
    for copy in copies:
        copy.start()
    far_index = at[1] ^ (lax.axis_size("sp") // 2)
    for n, (near_row, far_row, based) in enumerate(groups):
        weights, mine, theirs = refs[3 * n : 3 * n + 3]
        rows = weights.shape[0]
        own, other = column_of(weights, at[1]), column_of(weights, far_index)
        if n == 0:
            copies[0].wait()
        a = jnp.dot(mine[near_row : near_row + rows], near_w[...], preferred_element_type=jnp.float32)
        if n == 0:
            for copy in copies[1:]:
                copy.wait()
        b = jnp.dot(theirs[far_row : far_row + rows], far_w[...], preferred_element_type=jnp.float32)
        both = own * a.astype(jnp.bfloat16).astype(jnp.float32)
        both += other * b.astype(jnp.bfloat16).astype(jnp.float32)
        if based:
            both += refs[3 * members][:, column : column + extent].astype(jnp.float32)
        outs[n][...] = both.astype(outs[n].dtype)


def down_of(members, near, pieces, column, base=None):
    groups, operands, outs = [], [], []
    depth, extent = near.shape[0], pieces[0].shape[1] * len(pieces)
    for weights, near_h, near_row, far_h, far_row in members:
        groups.append((near_row, far_row, base is not None))
        operands += [weights, near_h, far_h]
        kind = jnp.bfloat16 if base is None else jnp.float32
        outs.append(jax.ShapeDtypeStruct((weights.shape[0], extent), kind))
    operands += [] if base is None else [base]
    flops = sum(4 * m[0].shape[0] * depth * extent for m in members)
    kernel = functools.partial(down_kernel, tuple(groups), column)
    scratch = [pltpu.VMEM((depth, extent), jnp.bfloat16)] * 2
    return call(kernel, outs, scratch, 5, flops, near, *pieces, *operands)


def quarter(array, axis, begin, extent):
    part = extent // lax.axis_size("tp")
    return lax.dynamic_slice_in_dim(array, begin + lax.axis_index("tp") * part, part, axis)


def share_square(mix, res_in, moe_gain, dense, expert_gate, expert_up, expert_down):
    far = lax.axis_size("sp") // 2
    across, along = 1, 2
    gate, up, down = expert_gate[0], expert_up[0], expert_down[0]
    depth, width = gate.shape[0], down.shape[1]
    cut = width // 2

    gate_q = swap(quarter(gate, 0, 0, depth), "sp", far)
    up_q = swap(quarter(up, 0, 0, depth), "sp", far)

    mixed, dense = mix(dense)
    others = [dense] + [swap(dense, "sp", b) for b in (across, along, across | along)]

    residual, low, high = mixed(res_in, moe_gain)
    x_high = swap(high, "sp", across)
    z_low = swap(low, "sp", along)
    x_low = swap(low, "sp", across)
    z_high = swap(high, "sp", along)

    far_gate = spread_tp(after(gate_q, low))
    lo_q = swap(quarter(down, 1, 0, cut), "sp", far)
    near = hidden_of([low, high], [gate], [up])
    x_high, z_low = after((x_high, z_low), near)
    d_high = swap(x_high, "sp", along)
    d_low = swap(z_low, "sp", across)
    up_q = after(up_q, z_low)
    hi_q = swap(quarter(down, 1, cut, cut), "sp", far)
    far_up = spread_tp(up_q)
    near_xz = hidden_of([x_low, x_high, z_low, z_high], [gate], [up])
    far_lo = spread_tp(after(lo_q, near_xz))
    near_d = hidden_of([d_low, d_high], [gate], [up])
    far_hi = spread_tp(after(hi_q, near_xz))
    tokens = [low, high, x_low, x_high, z_low, z_high, d_low, d_high]
    far_h = hidden_of(tokens, far_gate, far_up)

    rows = res_in.shape[0]
    to_x = (others[1], near_xz, 0, far_h, rows)
    to_z = (others[2], near_xz, rows, far_h, 2 * rows)
    to_d = (others[3], near_d, 0, far_h, 3 * rows)
    sums = []
    for column, pieces in ((0, far_lo), (cut, far_hi)):
        for_d, for_x, for_z = down_of([to_d, to_x, to_z], down, pieces, column)
        got_d = swap(for_d, "sp", across | along)
        got_x = swap(for_x, "sp", across)
        got_z = swap(for_z, "sp", along)
        (base,) = down_of([(others[0], near, 0, far_h, 0)], down, pieces, column, residual)
        total = base + (got_x.astype(jnp.float32) + got_z.astype(jnp.float32)) + got_d.astype(jnp.float32)
        sums.append(total.astype(jnp.bfloat16))
    return jnp.concatenate(sums, axis=1)


def body(
    residual_in,
    gate_outer,
    gate_inner,
    conv_input,
    conv_taps,
    norm_gain,
    out_weight,
    moe_gain,
    expert_ids,
    group_prob,
    route_prob,
    expert_gate,
    expert_up,
    expert_down,
):
    weights = group_prob[:, None] * route_prob / jnp.sum(route_prob, axis=1, keepdims=True)
    local_count, group_count = expert_gate.shape[0], lax.axis_size("sp")
    few = local_count * group_count <= 4 * expert_ids.shape[1]
    square = local_count == 1 and group_count % 8 == 0 and lax.axis_size("tp") == 4
    if not (few and square):
        mixed_out = mixer(gate_outer, gate_inner, conv_input, conv_taps)
        gathered = lax.all_to_all(mixed_out, "tp", split_axis=0, concat_axis=1, tiled=True)
        full_weight = lax.all_gather(out_weight, "tp", axis=0, tiled=True)
        full_gain = lax.all_gather(norm_gain, "tp", axis=0, tiled=True)
        normed = rms_norm(gathered, full_gain).astype(jnp.bfloat16)
        projected = jnp.dot(normed, full_weight, preferred_element_type=jnp.float32)
        residual = (residual_in.astype(jnp.float32) + projected).astype(jnp.bfloat16)
        routed_in = rms_norm(residual, moe_gain).astype(jnp.bfloat16)
        return route_slots(
            routed_in, residual, expert_ids, weights, expert_gate, expert_up, expert_down
        )
    lanes = jnp.arange(128, dtype=jnp.int32)[None]
    dense = sum(
        jnp.where(expert_ids[:, k : k + 1] == lanes, weights[:, k : k + 1], 0.0)
        for k in range(expert_ids.shape[1])
    )

    def mix(dense):
        mixed_out = mixer(gate_outer, gate_inner, conv_input, conv_taps)
        pieces = spread_tp(out_weight, mixed_out)
        parts = lax.axis_size("tp")
        blocks = mixed_out.reshape(parts, -1, mixed_out.shape[1])
        gain = jnp.broadcast_to(norm_gain, (parts, 16, norm_gain.shape[0]))
        blocks = jnp.concatenate([blocks, gain], axis=1)
        blocks = lax.all_to_all(blocks, "tp", split_axis=0, concat_axis=0)
        dense = after(dense, mixed_out)
        return functools.partial(project, blocks, pieces), dense

    return share_square(mix, residual_in, moe_gain, dense, expert_gate, expert_up, expert_down)


def solution(mesh):
    in_specs = (
        P(("sp", "tp"), None),
        P("sp", "tp"),
        P("sp", "tp"),
        P("sp", "tp"),
        P(None, "tp"),
        P("tp"),
        P("tp", None),
        P(),
        P(("sp", "tp"), None),
        P(("sp", "tp")),
        P(("sp", "tp"), None),
        P("sp", None, None),
        P("sp", None, None),
        P("sp", None, None),
    )
    out_specs = P(("sp", "tp"), None)
    return jax.shard_map(body, mesh=mesh, in_specs=in_specs, out_specs=out_specs, check_vma=False)
```
